256 devices in a mesh: sp: 64 (over z, x, core), tp: 4 (over y).
Axes of the slice: x: 4, y: 4, z: 8, core: 2. Of those that a mesh axis runs over, the one named last changes fastest.
Arguments:
- stream_in: bfloat16 [16384, 2048], P(('sp', 'tp')), may hold values from -6 to 6
- queries: bfloat16 [16384, 1024], P('sp', 'tp'), may hold values from -48 to 48
- keys: bfloat16 [16384, 512], P('sp', 'tp'), may hold values from -48 to 48
- values: bfloat16 [16384, 512], P('sp', 'tp'), may hold values from -6 to 6
- query_gain: float32 [64], replicated, may hold values from 1.5 to 6
- key_gain: float32 [64], replicated, may hold values from 1.5 to 6
- out_rows: bfloat16 [1024, 2048], P('tp'), may hold values from -0.1875 to 0.1875
- norm_gain: float32 [2048], replicated, may hold values from 0.1 to 1.9
- route_ids: int32 [16384, 2], P(('sp', 'tp')), may hold values from 0 to 63, all different within a row; in each aligned block of 64 rows (0 to 63, 64 to 127, ...) at most 3 rows name the same one
- route_weights: float32 [16384, 2], P(('sp', 'tp')), may hold values from 0.25 to 1
- gate_weight: bfloat16 [64, 2048, 3072], P('sp', None, 'tp'), may hold values from -0.125 to 0.125
- up_weight: bfloat16 [64, 2048, 3072], P('sp', None, 'tp'), may hold values from -0.125 to 0.125
- down_weight: bfloat16 [64, 3072, 2048], P('sp', 'tp'), may hold values from -0.109375 to 0.109375
Outputs:
- stream_out: bfloat16 [16384, 2048], P(('sp', 'tp'))
The draws below stay inside these ranges and needn't reach their ends.
Inputs may be any that keep to these rules, and one draw needn't show every extreme that they name: `route_ids`: each row names 2 different experts; among the rows of one device no expert is named more than 3 times.
All inputs are finite; a program needn't handle non-finite values.
Results may differ from the reference program's by a relative error of at most 0.014.
The reference program's roundings to bfloat16 on the way count: a program that leaves them out, or rounds other values in their place, can miss the bound.
Values may be sent and summed in bfloat16 or wider, within the bound.
No kernel may reach another device: no remote copies, remote signals or barrier semaphores. Data moves between devices by JAX's collectives and lax.ppermute only.
A program may use at most 128 MiB of HBM per device.

```python
import math
import jax
import jax.numpy as jnp
import numpy as np
from jax import lax

D = 2048
QUERY_HEAD_COUNT = 16
KEY_VALUE_HEADS = 8
HEAD_DIMENSION = 64
FF = 3072
TOPK = 2
GRID_W = 64
SEQ_LEN = 16384
TOTAL_TOKENS = 16384
TL = 64
ATTN_W = 1024
EXPERTS = 64
CAP = 3
N_SP = 64
N_TP = 4


def unrotated_rows(key, width):
    unrotated = jnp.clip(jax.random.normal(key, (TOTAL_TOKENS, width), jnp.float32), -6.0, 6.0)
    return unrotated


def draw_queries(key, part):
    unrotated = unrotated_rows(jax.random.fold_in(key, 11), QUERY_HEAD_COUNT * HEAD_DIMENSION)
    return unrotated.astype(jnp.bfloat16)


def draw_keys(key, part):
    unrotated = unrotated_rows(jax.random.fold_in(key, 21), KEY_VALUE_HEADS * HEAD_DIMENSION)
    return unrotated.astype(jnp.bfloat16)


def gain_table(key):
    spread = jax.random.uniform(key, (HEAD_DIMENSION,), jnp.float32, 1.5, 2.5)
    return spread


def draw_query_gain(key, part):
    return gain_table(jax.random.fold_in(key, 31))


def draw_key_gain(key, part):
    return gain_table(jax.random.fold_in(key, 37))


def block_levels(key, dims, shards, smallest, top_value):
    level, own = 1.0, jax.random.fold_in(key, 6)
    for dim, blocks in shards:
        steps = jnp.exp(jax.random.uniform(jax.random.fold_in(own, dim), (blocks,), jnp.float32, smallest / len(shards), top_value / len(shards)))
        level = level * jnp.repeat(steps, dims[dim] // blocks).reshape([-1 if axis == dim else 1 for axis in range(len(dims))])
    return level


def routed_block(rng, own, number, rows, amount, top, limit, lean):
    order = jax.random.permutation(rng, amount)
    crowded, ordinary = portions_of(amount, rows * top, limit, lean, True), portions_of(amount, rows * top, limit, lean, False)
    places = jnp.arange(amount)

    def named(tallies, turn):
        used = int((tallies > 0).sum())
        fixed = max(1, used // 4)
        passed = fixed + (places - fixed + turn * (used - fixed)) % max(1, amount - fixed)
        return jnp.zeros((amount,), jnp.int32).at[order[jnp.where(places < fixed, places, passed)]].set(jnp.asarray(tallies, jnp.int32))

    tallies = jnp.where(number % 4 == 0, named(crowded, number // 4), named(ordinary, number - number // 4 - 1))
    mixed = jax.random.permutation(jax.random.fold_in(own, 3), amount)
    donor, receiver = mixed[0:amount // 2 * 2:2], mixed[1:amount // 2 * 2:2]
    slack = jnp.minimum(tallies[donor] - 1, limit - tallies[receiver]) // 2
    slack = jnp.where((donor == order[0]) | (receiver == order[0]) | (tallies[receiver] == 0), 0, jnp.maximum(slack, 0))
    passed = jax.random.randint(jax.random.fold_in(own, 4), (amount // 2,), 0, 1 << 20) % (slack + 1)
    tallies = tallies.at[donor].add(-passed).at[receiver].add(passed)
    labels = jnp.searchsorted(jnp.cumsum(tallies), jnp.arange(rows * top), side="right").astype(jnp.int32)
    listing = labels.reshape(top, rows).T
    listing = listing[jax.random.permutation(jax.random.fold_in(own, 1), rows)]
    turn = jax.random.randint(jax.random.fold_in(own, 2), (rows, 1), 0, top)
    return jnp.take_along_axis(listing, (jnp.arange(top)[None, :] + turn) % top, axis=1)


def portions_of(amount, total, limit, lean, full):
    portions = [(1 << 20) // math.isqrt(grade ** lean) + 1 for grade in range(1, amount + 1)]
    largest = limit if full else min(limit, max(-(-total // amount), total * portions[0] // sum(portions)))
    least = 1 if total - largest >= amount - 1 else 0
    given, surplus = [largest] + [least] * (amount - 1), total - largest - least * (amount - 1)
    while surplus > 0:
        free = [i for i in range(1, amount) if given[i] < largest] or [i for i in range(1, amount) if given[i] < limit]
        mass, remaining = sum([portions[i] for i in free]), surplus
        for i in free:
            more = min(limit - given[i], max(1, remaining * portions[i] // mass), surplus)
            given[i] = given[i] + more
            surplus = surplus - more
    return np.array(given)


def noise(stream_key, dims, scale, bound, pieces=(), kind=jnp.bfloat16):
    values = scale * jax.random.normal(stream_key, dims, jnp.float32)
    if pieces:
        values = values * block_levels(stream_key, dims, pieces, -0.22, 0.18)
    return jnp.clip(values, -bound, bound).astype(kind)


def setup_inputs(seed: int = 0) -> dict:
    seeds = jax.random.split(jax.random.key(seed), 14)
    stream_in = noise(seeds[0], (TOTAL_TOKENS, D), 1.0, 6.0, ((0, 256),))
    queries = draw_queries(jax.random.fold_in(seeds[13], 71), 0)
    keys = draw_keys(jax.random.fold_in(seeds[13], 71), 0)
    values = noise(seeds[3], (TOTAL_TOKENS, KEY_VALUE_HEADS * HEAD_DIMENSION), 1.0, 6.0, ((0, 64), (1, 4)))
    query_gain = draw_query_gain(jax.random.fold_in(seeds[13], 71), 0)
    key_gain = draw_key_gain(jax.random.fold_in(seeds[13], 71), 0)
    out_rows = noise(seeds[6], (ATTN_W, D), ATTN_W ** -0.5, 0.1875, ((0, 4),))
    norm_gain = jnp.clip(1.0 + 0.18 * jax.random.normal(seeds[7], (D,), jnp.float32), 0.1, 1.9)
    route_ids_keys = jax.random.split(jax.random.fold_in(seeds[8], 1), TOTAL_TOKENS // TL)
    route_ids_turns = jax.random.permutation(jax.random.fold_in(seeds[8], 3), TOTAL_TOKENS // TL)
    route_ids = jax.vmap(lambda own, number: routed_block(jax.random.fold_in(seeds[8], 2), own, number, TL, EXPERTS, TOPK, CAP, 2))(route_ids_keys, route_ids_turns).reshape((TOTAL_TOKENS, TOPK))
    route_weights = jnp.clip(0.25 + 0.75 * jax.random.uniform(seeds[9], (TOTAL_TOKENS, TOPK), jnp.float32) ** block_levels(seeds[9], (TOTAL_TOKENS, TOPK), ((0, 256),), -0.2, 0.2), 0.25, 1.0)
    gate_weight = noise(seeds[10], (EXPERTS, D, FF), D ** -0.5, 0.125, ((0, 64), (2, 4)))
    up_weight = noise(seeds[11], (EXPERTS, D, FF), D ** -0.5, 0.125, ((0, 64), (2, 4)))
    down_weight = noise(seeds[12], (EXPERTS, FF, D), FF ** -0.5, 0.109375, ((0, 64), (1, 4)))
    return {"stream_in": stream_in, "queries": queries, "keys": keys, "values": values, "query_gain": query_gain, "key_gain": key_gain, "out_rows": out_rows, "norm_gain": norm_gain, "route_ids": route_ids, "route_weights": route_weights, "gate_weight": gate_weight, "up_weight": up_weight, "down_weight": down_weight}


EPS = 1e-06
THETA = 10000.0

def turn_tables(offset, count, head_size):
    position = offset + jnp.arange(count, dtype=jnp.int32)
    grid_row = (position // GRID_W).astype(jnp.float32)
    column = (position % GRID_W).astype(jnp.float32)
    pair_index = jnp.arange(head_size // 4, dtype=jnp.float32)
    inverse = THETA ** (-4.0 * pair_index / head_size)
    angles = jnp.concatenate([grid_row[:, None] * inverse, column[:, None] * inverse], axis=1)
    return (jnp.cos(angles), jnp.sin(angles))

def normalize_rotate(block_data, gain_vector, cos_table, sin_table):
    row_count = block_data.shape[0]
    head_size = gain_vector.shape[0]
    wide = block_data.astype(jnp.float32).reshape(row_count, -1, head_size)
    wide = wide * lax.rsqrt(lax.optimization_barrier(jnp.mean(wide * wide, axis=-1, keepdims=True)) + EPS) * gain_vector
    pairs = wide.reshape(row_count, wide.shape[1], head_size // 2, 2)
    even_part = pairs[..., 0]
    odd_part = pairs[..., 1]
    cosine = cos_table[:, None, :]
    sine_part = sin_table[:, None, :]
    turned = jnp.stack([even_part * cosine - odd_part * sine_part, even_part * sine_part + odd_part * cosine], axis=-1)
    return turned.reshape(row_count, -1).astype(jnp.bfloat16)

def attend(rotated_queries, rotated_keys, values):
    sequence_length = rotated_queries.shape[0]
    group_head_count = QUERY_HEAD_COUNT // KEY_VALUE_HEADS
    rows_per_block = math.gcd(sequence_length, 128)
    blocked_queries = rotated_queries.reshape(sequence_length // rows_per_block, rows_per_block, KEY_VALUE_HEADS, group_head_count, HEAD_DIMENSION).astype(jnp.float32)
    every_key_row = rotated_keys.reshape(sequence_length, KEY_VALUE_HEADS, HEAD_DIMENSION).astype(jnp.float32)
    every_value_row = values.reshape(sequence_length, KEY_VALUE_HEADS, HEAD_DIMENSION).astype(jnp.float32)

    def one_block(query_block):
        scores = jnp.einsum('qkgd,skd->qkgs', query_block, every_key_row) * HEAD_DIMENSION ** (-0.5)
        row_top = lax.optimization_barrier(jnp.max(scores, axis=-1, keepdims=True))
        weights = jnp.exp(scores - row_top)
        row_total = lax.optimization_barrier(jnp.sum(weights, axis=-1))
        probs = lax.optimization_barrier(weights.astype(jnp.bfloat16)).astype(jnp.float32)
        mixed_rows = jnp.einsum('qkgs,skd->qkgd', probs, every_value_row) / row_total[..., None]
        return mixed_rows.astype(jnp.bfloat16).reshape(rows_per_block, QUERY_HEAD_COUNT * HEAD_DIMENSION)
    return lax.map(one_block, blocked_queries).reshape(sequence_length, QUERY_HEAD_COUNT * HEAD_DIMENSION)

def reference(stream_in, queries, keys, values, query_gain, key_gain, out_rows, norm_gain, route_ids, route_weights, gate_weight, up_weight, down_weight):
    sequence_length = queries.shape[0]
    sequence_count = sequence_length // SEQ_LEN
    cos_one, sin_one = turn_tables(0, SEQ_LEN, HEAD_DIMENSION)
    cos_table = jnp.tile(cos_one, (sequence_count, 1))
    sin_table = jnp.tile(sin_one, (sequence_count, 1))
    rotated_queries = normalize_rotate(queries, query_gain, cos_table, sin_table)
    rotated_keys = normalize_rotate(keys, key_gain, cos_table, sin_table)

    def one_sequence(triple):
        return attend(triple[0], triple[1], triple[2])
    attended = lax.map(one_sequence, (rotated_queries.reshape(sequence_count, SEQ_LEN, -1), rotated_keys.reshape(sequence_count, SEQ_LEN, -1), values.reshape(sequence_count, SEQ_LEN, -1)))
    attended = attended.reshape(sequence_length, QUERY_HEAD_COUNT * HEAD_DIMENSION)
    projected = jnp.dot(attended, out_rows, preferred_element_type=jnp.float32)
    stream = (stream_in.astype(jnp.float32) + projected).astype(jnp.bfloat16)
    stream_wide = stream.astype(jnp.float32)
    normed = (stream_wide * lax.rsqrt(lax.optimization_barrier(jnp.mean(stream_wide * stream_wide, axis=1, keepdims=True)) + EPS) * norm_gain).astype(jnp.bfloat16)
    flat_ids = route_ids.reshape(-1).astype(jnp.int32)
    total_routes = flat_ids.shape[0]
    most_rows = N_SP * N_TP * CAP
    ordering = jnp.argsort(flat_ids, stable=True).astype(jnp.int32)
    counts = lax.optimization_barrier(jnp.sum((flat_ids[:, None] == jnp.arange(EXPERTS, dtype=jnp.int32)[None, :]).astype(jnp.int32), axis=0)).astype(jnp.int32)
    starts = (jnp.cumsum(counts) - counts).astype(jnp.int32)
    padded = jnp.concatenate([ordering, jnp.zeros((most_rows,), jnp.int32)])
    group_width = FF // N_TP

    def for_expert(results, expert):
        begin = starts[expert].astype(jnp.int32)
        chosen = lax.dynamic_slice(padded, (begin,), (most_rows,))
        valid = jnp.arange(most_rows, dtype=jnp.int32) < counts[expert]
        rows = normed[chosen // TOPK]
        gate_value = jnp.dot(rows, gate_weight[expert], preferred_element_type=jnp.float32)
        up_value = jnp.dot(rows, up_weight[expert], preferred_element_type=jnp.float32)
        hidden = (jax.nn.silu(gate_value) * up_value).astype(jnp.bfloat16)
        partials = jnp.einsum('rgf,gfd->rgd', hidden.reshape(most_rows, N_TP, group_width).astype(jnp.float32), down_weight[expert].reshape(N_TP, group_width, D).astype(jnp.float32))
        partials = lax.optimization_barrier(partials.astype(jnp.bfloat16)).astype(jnp.float32)
        answer = lax.optimization_barrier(jnp.sum(partials, axis=1)).astype(jnp.bfloat16)
        slot_index = jnp.where(valid, chosen, total_routes)
        return (results.at[slot_index].set(answer, mode='drop'), None)
    results = jnp.zeros((total_routes, D), jnp.bfloat16)
    results = lax.scan(for_expert, results, jnp.arange(EXPERTS, dtype=jnp.int32))[0]
    picked = results.reshape(sequence_length, TOPK, D).astype(jnp.float32)
    mixed_out = stream_wide + lax.optimization_barrier(jnp.sum(route_weights[:, :, None] * picked, axis=1))
    return mixed_out.astype(jnp.bfloat16)
```

```python
import jax
import jax.numpy as jnp
from jax import lax
from jax.experimental import pallas as pl
from jax.experimental.pallas import tpu as pltpu
from jax.sharding import PartitionSpec as P

GRID_W = 64
EPS = 1e-06
THETA = 10000.0
NZ, NX, NC = 8, 4, 2
BF16 = jnp.bfloat16
F32 = jnp.float32
CAP = 3
OUT_ROWS = 272


VMEM = pl.BlockSpec(memory_space=pltpu.VMEM)
SMEM = pl.BlockSpec(memory_space=pltpu.SMEM)


def shift_z(x, d):
    return lax.ppermute(
        x, "sp", [(z * 8 + r, (z + d) % NZ * 8 + r) for z in range(NZ) for r in range(8)]
    )


def shift_x(x, d):
    return lax.ppermute(
        x,
        "sp",
        [
            (z * 8 + i * 2 + c, z * 8 + (i + d) % NX * 2 + c)
            for z in range(NZ)
            for i in range(NX)
            for c in range(NC)
        ],
    )


def swap_core(x):
    return lax.ppermute(x, "sp", [(i, i ^ 1) for i in range(64)])


def shift_y(x, d):
    return lax.ppermute(x, "tp", [(i, (i + d) % 4) for i in range(4)])


def call(kernel, out_shape, n_in, scratch=(), specs=None, **kw):
    return pl.pallas_call(
        kernel,
        out_shape=out_shape,
        in_specs=specs or [VMEM] * n_in,
        out_specs=jax.tree.map(lambda _: VMEM, out_shape),
        scratch_shapes=list(scratch),
        compiler_params=pltpu.CompilerParams(vmem_limit_bytes=58 * 1024 * 1024),
        **kw,
    )


def turn_tables(offset, count, head_size):
    position = offset + jnp.arange(count, dtype=jnp.int32)
    grid_row = (position // GRID_W).astype(F32)
    column = (position % GRID_W).astype(F32)
    pair_index = jnp.arange(head_size // 4, dtype=F32)
    inverse = THETA ** (-4.0 * pair_index / head_size)
    angles = jnp.concatenate([inverse[:, None] * grid_row, inverse[:, None] * column], axis=0)
    cosine = jnp.repeat(jnp.cos(angles), 2, axis=0)
    sine = jnp.sin(angles)
    return cosine, jnp.stack([-sine, sine], axis=1).reshape(head_size, count)


def prep_kernel(q_ref, k_ref, v_ref, qg_ref, kg_ref, cos_ref, sin_ref, qt_ref, kv_ref):
    cosine = cos_ref[...]
    sine = sin_ref[...]
    even = lax.broadcasted_iota(jnp.int32, (64, 256), 0) % 2 == 0

    def turned(head, gain):
        mean = jnp.mean(head * head, axis=0, keepdims=True)
        wide = head * lax.rsqrt(mean + EPS) * gain
        other = jnp.where(even, pltpu.roll(wide, 63, 0), pltpu.roll(wide, 1, 0))
        return wide * cosine + other * sine

    qt = q_ref[...].astype(F32).T
    for h in range(4):
        head = turned(qt[h * 64 : (h + 1) * 64], qg_ref[...])
        qt_ref[h * 64 : (h + 1) * 64, :] = (head * 0.125).astype(BF16)
    kt = k_ref[...].astype(F32).T
    k_heads = [turned(kt[h * 64 : (h + 1) * 64], kg_ref[...]) for h in range(2)]
    kv_ref[0:256, :] = jnp.concatenate(k_heads, axis=0).T.astype(BF16)
    vt = v_ref[...].astype(F32).T
    kv_ref[256:384, :] = vt[:, 0:128].astype(BF16)
    kv_ref[384:512, :] = vt[:, 128:256].astype(BF16)


def flash_kernel(nq, nkv, *refs):
    q_refs = refs[:nq]
    kv_refs = refs[nq : nq + nkv]
    o_refs = refs[nq + nkv : nq + nkv + nq]
    qpad, vext, s_buf, o_buf, l_buf = refs[nq + nkv + nq :]
    steps = nq * 4
    for b in range(nq):
        for h in range(4):
            g = h // 2
            qpad[b * 4 + h, g * 64 : (g + 1) * 64, :] = q_refs[b][h * 64 : (h + 1) * 64, :]
            qpad[b * 4 + h, (1 - g) * 64 : (2 - g) * 64, :] = jnp.zeros((64, 256), BF16)
    for i in range(nkv):
        for g in range(2):
            for half in range(2):
                vext[g, 0:64, i * 256 + half * 128 : i * 256 + (half + 1) * 128] = kv_refs[i][
                    256 + half * 128 + g * 64 : 256 + half * 128 + (g + 1) * 64, :
                ]
    vext[:, 64:80, :] = jnp.ones((2, 16, nkv * 256), BF16)

    def score(step, slot, i):
        s = jnp.dot(kv_refs[i][0:256, :], qpad[step], preferred_element_type=F32)
        s_buf[slot, i * 256 : (i + 1) * 256, :] = s
        return jnp.max(s.reshape(32, 8, 256), axis=0)

    def finish(step, top, acc):
        total = acc[64:65, :]
        o_buf[step] = (acc[0:64, :] / total).astype(BF16)
        l_buf[step] = jnp.broadcast_to(top + jnp.log(total), (8, 256))

    first = score(0, 0, 0)
    for i in range(1, nkv):
        first = jnp.maximum(first, score(0, 0, i))

    def body(step, folded):
        slot = lax.rem(step, 2)
        following = jnp.minimum(step + 1, steps - 1)
        g = lax.rem(step, 4) // 2
        top = jnp.max(folded, axis=0, keepdims=True)
        acc = jnp.zeros((80, 256), F32)
        nxt = None
        for i in range(nkv):
            m = score(following, 1 - slot, i)
            nxt = m if nxt is None else jnp.maximum(nxt, m)
            p = jnp.exp(s_buf[slot, i * 256 : (i + 1) * 256, :] - top).astype(BF16)
            acc = acc + jnp.dot(
                vext[g, :, i * 256 : (i + 1) * 256], p, preferred_element_type=F32
            )
        finish(step, top, acc)
        return nxt

    lax.fori_loop(0, steps, body, first)
    for b in range(nq):
        for h in range(4):
            o_refs[b][h * 64 : (h + 1) * 64, :] = o_buf[b * 4 + h]
        lse = jnp.concatenate([l_buf[b * 4 + h, 0:1, :] for h in range(4)], axis=0)
        high = lse.astype(BF16)
        rest = lse - high.astype(F32)
        middle = rest.astype(BF16)
        low = (rest - middle.astype(F32)).astype(BF16)
        parts = jnp.concatenate(
            [high.astype(F32), middle.astype(F32), low.astype(F32), jnp.zeros((4, 256), F32)], axis=0
        )
        o_refs[b][256:272, :] = parts.astype(BF16)


def flash(qs, kvs):
    nq, nkv = len(qs), len(kvs)
    return call(
        lambda *refs: flash_kernel(nq, nkv, *refs),
        [jax.ShapeDtypeStruct((OUT_ROWS, 256), BF16)] * nq,
        nq + nkv,
        [
            pltpu.VMEM((nq * 4, 128, 256), BF16),
            pltpu.VMEM((2, 80, nkv * 256), BF16),
            pltpu.VMEM((2, nkv * 256, 256), F32),
            pltpu.VMEM((nq * 4, 64, 256), BF16),
            pltpu.VMEM((nq * 4, 8, 256), F32),
        ],
        name="flash",
    )(*qs, *kvs)


def merge_kernel(n, y_ref, *refs):
    parts = refs[:n]
    outs = refs[n : n + 4]
    buf = refs[n + 4]
    stats = [p[256:272, :].astype(F32) for p in parts]
    for h in range(4):
        lse = [s[h : h + 1] + s[4 + h : 5 + h] + s[8 + h : 9 + h] for s in stats]
        top = lse[0]
        for v in lse[1:]:
            top = jnp.maximum(top, v)
        total = jnp.zeros((1, 256), F32)
        acc = jnp.zeros((64, 256), F32)
        for p, v in zip(parts, lse):
            w = jnp.exp(v - top)
            total = total + w
            acc = acc + p[h * 64 : (h + 1) * 64, :].astype(F32) * w
        buf[h * 64 : (h + 1) * 64, :] = acc / total
    rows = buf[...].T
    buf[...] = rows
    y = y_ref[0]
    for d in range(4):
        start = pl.multiple_of(lax.rem(y + d, 4) * 64, 64)
        outs[d][...] = buf[pl.ds(start, 64), :].astype(BF16)


def route_kernel(col_ref, row_ref, placed_ref):
    col = col_ref[...]
    same = jnp.broadcast_to(col, (128, 128)) == jnp.broadcast_to(row_ref[...], (128, 128))
    earlier = lax.broadcasted_iota(jnp.int32, (128, 128), 1) < lax.broadcasted_iota(
        jnp.int32, (128, 128), 0
    )
    rank = jnp.sum(jnp.where(same & earlier, 1.0, 0.0), axis=1, keepdims=True).astype(jnp.int32)
    lane = lax.broadcasted_iota(jnp.int32, (128, CAP * 64), 1)
    target = rank * 64 + col
    placed_ref[...] = jnp.where(lane == target, 1.0, 0.0).astype(BF16)


def project_kernel(a0, a1, a2, a3, w0, w1, w2, w3, in_ref, gain_ref, placed_ref, stream_ref, out_ref):
    acc = jnp.dot(a0[...], w0[...], preferred_element_type=F32)
    for a, w in ((a1, w1), (a2, w2), (a3, w3)):
        acc = acc + jnp.dot(a[...], w[...], preferred_element_type=F32)
    stream = (in_ref[...].astype(F32) + acc).astype(BF16)
    stream_ref[...] = stream
    wide = stream.astype(F32)
    normed = wide * lax.rsqrt(jnp.mean(wide * wide, axis=1, keepdims=True) + EPS) * gain_ref[...]
    normed = normed.astype(BF16)
    both = jnp.concatenate([normed, normed], axis=0)
    for s in range(CAP):
        picked = lax.dot_general(
            placed_ref[:, s * 64 : (s + 1) * 64],
            both,
            (((0,), (0,)), ((), ())),
            preferred_element_type=F32,
        )
        out_ref[:, s * 2048 : (s + 1) * 2048] = picked.astype(BF16)


def expert_kernel(n, *refs):
    rows = refs[:n]
    gate_ref, up_ref, down_ref = refs[n : n + 3]
    outs = refs[n + 3 : 2 * n + 3]
    x_buf, acc = refs[2 * n + 3 :]
    step = pl.program_id(0)
    last = pl.num_programs(0) - 1

    @pl.when(step == 0)
    def _():
        for j in range(n):
            for s in range(CAP):
                x_buf[(j * CAP + s) * 64 : (j * CAP + s + 1) * 64, :] = rows[j][
                    :, s * 2048 : (s + 1) * 2048
                ]

    x = x_buf[...]
    gate = jnp.dot(x, gate_ref[...], preferred_element_type=F32)
    up = jnp.dot(x, up_ref[...], preferred_element_type=F32)
    hidden = (gate / (1.0 + jnp.exp(-gate)) * up).astype(BF16)
    part = jnp.dot(hidden, down_ref[...], preferred_element_type=F32)

    @pl.when(step == 0)
    def _():
        acc[...] = part

    @pl.when(step > 0)
    def _():
        acc[...] = acc[...] + part

    @pl.when(step == last)
    def _():
        for j in range(n):
            for s in range(CAP):
                outs[j][:, s * 2048 : (s + 1) * 2048] = acc[
                    (j * CAP + s) * 64 : (j * CAP + s + 1) * 64, :
                ].astype(BF16)


def experts(rows, gate, up, down):
    n = len(rows)
    wide = 256
    whole = pl.BlockSpec((64, CAP * 2048), lambda i: (0, 0))
    return pl.pallas_call(
        lambda *refs: expert_kernel(n, *refs),
        grid=(768 // wide,),
        out_shape=[jax.ShapeDtypeStruct((64, CAP * 2048), BF16)] * n,
        in_specs=[whole] * n
        + [
            pl.BlockSpec((2048, wide), lambda i: (0, i)),
            pl.BlockSpec((2048, wide), lambda i: (0, i)),
            pl.BlockSpec((wide, 2048), lambda i: (i, 0)),
        ],
        out_specs=[whole] * n,
        scratch_shapes=[
            pltpu.VMEM((n * CAP * 64, 2048), BF16),
            pltpu.VMEM((n * CAP * 64, 2048), F32),
        ],
        compiler_params=pltpu.CompilerParams(vmem_limit_bytes=58 * 1024 * 1024),
        name="experts",
    )(*rows, gate, up, down)


def sum_kernel(a, b, c, d, out):
    total = a[...].astype(F32) + b[...].astype(F32) + c[...].astype(F32) + d[...].astype(F32)
    out[...] = total.astype(BF16)


def final_kernel(back_ref, placed_ref, weight_ref, stream_ref, out_ref):
    picked = jnp.dot(
        placed_ref[:, 0:64], back_ref[:, 0:2048], preferred_element_type=F32
    )
    for s in range(1, CAP):
        picked = picked + jnp.dot(
            placed_ref[:, s * 64 : (s + 1) * 64],
            back_ref[:, s * 2048 : (s + 1) * 2048],
            preferred_element_type=F32,
        )
    weighted = picked[0:64] * weight_ref[:, 0:1] + picked[64:128] * weight_ref[:, 1:2]
    out_ref[...] = (stream_ref[...].astype(F32) + weighted).astype(BF16)


def local(
    stream_in,
    queries,
    keys,
    values,
    query_gain,
    key_gain,
    out_rows,
    norm_gain,
    route_ids,
    route_weights,
    gate_weight,
    up_weight,
    down_weight,
):
    sds = jax.ShapeDtypeStruct
    cosine, sine = turn_tables(lax.axis_index("sp") * 256, 256, 64)
    qt, kv = call(prep_kernel, [sds((256, 256), BF16), sds((512, 128), BF16)], 7, name="prep")(
        queries, keys, values, query_gain[:, None], key_gain[:, None], cosine, sine
    )
    far = shift_z(kv, 4)
    f1, b1 = shift_z(kv, 1), shift_z(kv, -1)
    q1, q3, q2 = shift_x(qt, 1), shift_x(qt, -1), shift_x(qt, 2)
    f2, b2 = shift_z(f1, 1), shift_z(b1, -1)
    f3, b3 = shift_z(f2, 1), shift_z(b2, -1)
    mine = [kv, f1, b1, far, f2, b2, f3, b3]
    kvs = mine + [swap_core(x) for x in mine]
    ids = route_ids.astype(jnp.int32).T.reshape(128)
    placed = call(route_kernel, sds((128, CAP * 64), BF16), 2, name="route")(
        ids[:, None], ids[None, :]
    )
    o2, o1, o3, o0 = flash([q2, q1, q3, qt], kvs)
    parts = [o0, shift_x(o1, -1), shift_x(o2, 2), shift_x(o3, 1)]
    y = lax.axis_index("tp").astype(jnp.int32).reshape(1)
    att = call(
        lambda *refs: merge_kernel(4, *refs),
        [sds((64, 256), BF16)] * 4,
        5,
        [pltpu.VMEM((256, 256), F32)],
        specs=[SMEM] + [VMEM] * 4,
        name="merge",
    )(y, *parts)
    att = [att[0]] + [shift_y(att[d], d) for d in (1, 2, 3)]
    rows_of = [out_rows] + [shift_y(out_rows, d) for d in (1, 2, 3)]
    stream, outgoing = call(
        project_kernel, [sds((64, 2048), BF16), sds((64, CAP * 2048), BF16)], 11, name="project"
    )(*att, *rows_of, stream_in, norm_gain[None, :], placed)

    arrived = lax.all_to_all(outgoing, "sp", 0, 0, tiled=True)
    weights = (gate_weight[0], up_weight[0], down_weight[0])
    r1, r3 = shift_y(arrived, 1), shift_y(arrived, 3)
    (p0,) = experts([arrived], *weights)
    r2 = jnp.concatenate([shift_y(r1[:32], 1), shift_y(r3[32:], 3)], axis=0)
    p1, p3 = experts([r1, r3], *weights)
    (p2,) = experts([r2], *weights)
    back = [p0, shift_y(p1, 3), shift_y(p2, 2), shift_y(p3, 1)]
    answer = call(sum_kernel, sds((64, CAP * 2048), BF16), 4, name="total")(*back)
    returned = lax.all_to_all(answer, "sp", 0, 0, tiled=True)
    return call(final_kernel, sds((64, 2048), BF16), 4, name="final")(
        returned, placed, route_weights, stream
    )


def solution(mesh):
    return jax.shard_map(
        local,
        mesh=mesh,
        in_specs=(
            P(("sp", "tp"), None),
            P("sp", "tp"),
            P("sp", "tp"),
            P("sp", "tp"),
            P(),
            P(),
            P("tp", None),
            P(),
            P(("sp", "tp"), None),
            P(("sp", "tp"), None),
            P("sp", None, "tp"),
            P("sp", None, "tp"),
            P("sp", "tp", None),
        ),
        out_specs=P(("sp", "tp"), None),
        check_vma=False,
    )
```
